32 devices in a mesh: sp: 16 (over z, y, core), tp: 2 (over x).
Axes of the slice: x: 2, y: 2, z: 4, core: 2. Of those that a mesh axis runs over, the one named last changes fastest.
Arguments:
- residual: bfloat16 [2048, 2048], P(('sp', 'tp')), may hold values from -6 to 6
- q_small: bfloat16 [2048, 1024], P('sp', 'tp'), may hold values from -6 to 6
- k_small: bfloat16 [2048, 1024], P('sp', 'tp'), may hold values from -6 to 6
- v_small: bfloat16 [2048, 1024], P('sp', 'tp'), may hold values from -6 to 6
- q_large: bfloat16 [2048, 1024], P('sp', 'tp'), may hold values from -6 to 6
- k_large: bfloat16 [2048, 1024], P('sp', 'tp'), may hold values from -6 to 6
- v_large: bfloat16 [2048, 1024], P('sp', 'tp'), may hold values from -6 to 6
- forget_small: float32 [2048, 16], P('sp', 'tp'), may hold values from 0 to 20
- forget_large: float32 [2048, 8], P('sp', 'tp'), may hold values from 0 to 20
- w_out_small: bfloat16 [1024, 2048], P('tp'), may hold values from -0.125 to 0.125
- w_out_large: bfloat16 [1024, 2048], P('tp'), may hold values from -0.125 to 0.125
- norm_gain: float32 [2048], replicated, may hold values from 0.1 to 1.9
- w_gate: bfloat16 [2048, 4096], P('sp', 'tp'), may hold values from -0.125 to 0.125
- w_up: bfloat16 [2048, 4096], P('sp', 'tp'), may hold values from -0.125 to 0.125
- conv_gate: float32 [3, 4096], P(None, 'tp'), may hold values from -3 to 3
- conv_up: float32 [3, 4096], P(None, 'tp'), may hold values from -3 to 3
- w_down: bfloat16 [4096, 2048], P('tp', 'sp'), may hold values from -0.09375 to 0.09375
Outputs:
- mixed: bfloat16 [2048, 2048], P(('sp', 'tp'))
The draws below stay inside these ranges and needn't reach their ends.
All inputs are finite; a program needn't handle non-finite values.
Results may differ from the reference program's by a relative error of at most 0.015.
Values may be sent and summed in bfloat16 or wider, within the bound.
A program may use at most 64 MiB of HBM per device.

```python
import math
import jax
import jax.numpy as jnp
from jax import lax

D = 2048
FF = 4096
HEADS_SMALL = 16
HEAD_SMALL = 64
HEADS_LARGE = 8
HEAD_LARGE = 128
TOK_DEV = 128
TOKENS = 2048


def draw_planted(key, salt, heads, size, phase):
    base = jnp.clip(jax.random.normal(jax.random.fold_in(key, salt), (TOKENS, heads * size), jnp.float32), -6.0, 6.0)
    return base.astype(jnp.bfloat16)


def draw_gates(key, salt, heads):
    order = jax.random.permutation(jax.random.fold_in(key, salt), heads)
    fast_count = heads // 2
    fast = order < fast_count
    level = jnp.where(fast, 4.0, math.log(TOKENS) + 1.0)
    noise = jnp.clip(jax.random.normal(jax.random.fold_in(key, salt + 1), (TOKENS, heads), jnp.float32), -3.0, 3.0)
    blocks = jax.random.uniform(jax.random.fold_in(key, salt + 2), (TOKENS // TOK_DEV, heads), jnp.float32, -0.7, 0.7)
    return (level[None, :] + noise + jnp.repeat(blocks, TOK_DEV, axis=0)).astype(jnp.float32)


def draw_q_small(key, part):
    return draw_planted(key, 11, HEADS_SMALL, HEAD_SMALL, 40)


def draw_k_small(key, part):
    return draw_planted(key, 12, HEADS_SMALL, HEAD_SMALL, 3)


def draw_q_large(key, part):
    return draw_planted(key, 13, HEADS_LARGE, HEAD_LARGE, 40)


def draw_k_large(key, part):
    return draw_planted(key, 14, HEADS_LARGE, HEAD_LARGE, 3)


def draw_forget_small(key, part):
    return draw_gates(key, 21, HEADS_SMALL)


def draw_forget_large(key, part):
    return draw_gates(key, 31, HEADS_LARGE)


def level_of(key, extent, cuts, least, high):
    level, own = 1.0, jax.random.fold_in(key, 6)
    for position, shards_of in cuts:
        draws = jnp.exp(jax.random.uniform(jax.random.fold_in(own, position), (shards_of,), jnp.float32, least / len(cuts), high / len(cuts)))
        level = level * jnp.repeat(draws, extent[position] // shards_of).reshape([-1 if axis == position else 1 for axis in range(len(extent))])
    return level


def bell_draw(stream_key, extent, deviation, bound, cuts=(), kind=jnp.bfloat16):
    values = jax.random.normal(stream_key, extent, jnp.float32) * deviation
    if len(cuts) > 0:
        values = level_of(stream_key, extent, cuts, -0.22, 0.18) * values
    return jnp.clip(values, min=-bound, max=bound).astype(kind)


def setup_inputs(seed: int = 0) -> dict:
    key_of = jax.random.split(jax.random.key(seed), 18)
    return {
        "residual": bell_draw(key_of[0], (TOKENS, D), 1.0, 6.0, ((0, 32),)),
        "q_small": draw_q_small(jax.random.fold_in(key_of[17], 71), 0),
        "k_small": draw_k_small(jax.random.fold_in(key_of[17], 71), 0),
        "v_small": bell_draw(key_of[3], (TOKENS, HEADS_SMALL * HEAD_SMALL), 1.0, 6.0, ((0, 16), (1, 2))),
        "q_large": draw_q_large(jax.random.fold_in(key_of[17], 71), 0),
        "k_large": draw_k_large(jax.random.fold_in(key_of[17], 71), 0),
        "v_large": bell_draw(key_of[6], (TOKENS, HEADS_LARGE * HEAD_LARGE), 1.0, 6.0, ((0, 16), (1, 2))),
        "forget_small": draw_forget_small(jax.random.fold_in(key_of[17], 71), 0),
        "forget_large": draw_forget_large(jax.random.fold_in(key_of[17], 71), 0),
        "w_out_small": bell_draw(key_of[9], (HEADS_SMALL * HEAD_SMALL, D), (HEADS_SMALL * HEAD_SMALL + HEADS_LARGE * HEAD_LARGE) ** -0.5, 0.125, ((0, 2),)),
        "w_out_large": bell_draw(key_of[10], (HEADS_LARGE * HEAD_LARGE, D), (HEADS_SMALL * HEAD_SMALL + HEADS_LARGE * HEAD_LARGE) ** -0.5, 0.125, ((0, 2),)),
        "norm_gain": jnp.clip(1.0 + 0.18 * jax.random.normal(key_of[11], (D,), jnp.float32), 0.1, 1.9),
        "w_gate": bell_draw(key_of[12], (D, FF), D ** -0.5, 0.125, ((0, 16), (1, 2))),
        "w_up": bell_draw(key_of[13], (D, FF), D ** -0.5, 0.125, ((0, 16), (1, 2))),
        "conv_gate": bell_draw(key_of[14], (3, FF), 0.577, 3.0, ((1, 2),), jnp.float32),
        "conv_up": bell_draw(key_of[15], (3, FF), 0.577, 3.0, ((1, 2),), jnp.float32),
        "w_down": bell_draw(key_of[16], (FF, D), FF ** -0.5, 0.09375, ((0, 2), (1, 16))),
    }


EPS = 1e-06
NEG = -1e+30

def group_attention(queries, keys, values, forget, heads, size):
    total = queries.shape[0]
    cumul = jnp.cumsum(jax.nn.log_sigmoid(forget.astype(jnp.float32)), axis=0)
    qf = queries.reshape(total, heads, size).astype(jnp.float32)
    kf = keys.reshape(total, heads, size).astype(jnp.float32)
    vf = values.reshape(total, heads, size).astype(jnp.float32)
    block = math.gcd(total, 128)
    kpos = jnp.arange(total, dtype=jnp.int32)
    scale = size ** (-0.5)

    def one_block(start):
        qb = lax.dynamic_slice_in_dim(qf, start, block, 0)
        cb = lax.dynamic_slice_in_dim(cumul, start, block, 0)
        qpos = start + jnp.arange(block, dtype=jnp.int32)
        scores = jnp.einsum('qhd,khd->qhk', qb, kf) * scale + cb[:, :, None] - cumul.T[None, :, :]
        keep = (kpos[None, :] <= qpos[:, None])[:, None, :]
        scores = jnp.where(keep, scores, NEG)
        top = lax.optimization_barrier(jnp.max(scores, axis=-1, keepdims=True))
        weights = jnp.where(keep, jnp.exp(scores - top), 0.0)
        denom = lax.optimization_barrier(jnp.sum(weights, axis=-1))
        wbf = weights.astype(jnp.bfloat16).astype(jnp.float32)
        attended = jnp.einsum('qhk,khd->qhd', wbf, vf) / denom[:, :, None]
        normed = attended * lax.rsqrt(lax.optimization_barrier(jnp.mean(attended * attended, axis=-1, keepdims=True)) + EPS)
        return normed.astype(jnp.bfloat16).reshape(block, heads * size)
    starts = (jnp.arange(total // block) * block).astype(jnp.int32)
    return lax.map(one_block, starts).reshape(total, heads * size)

def reference(residual, q_small, k_small, v_small, q_large, k_large, v_large, forget_small, forget_large, w_out_small, w_out_large, norm_gain, w_gate, w_up, conv_gate, conv_up, w_down):
    normed_small = group_attention(q_small, k_small, v_small, forget_small, HEADS_SMALL, HEAD_SMALL)
    normed_large = group_attention(q_large, k_large, v_large, forget_large, HEADS_LARGE, HEAD_LARGE)
    first = residual.astype(jnp.float32) + jnp.dot(normed_small, w_out_small, preferred_element_type=jnp.float32) + jnp.dot(normed_large, w_out_large, preferred_element_type=jnp.float32)
    normal = (first * lax.rsqrt(lax.optimization_barrier(jnp.mean(first * first, axis=-1, keepdims=True)) + EPS) * norm_gain.astype(jnp.float32)).astype(jnp.bfloat16)
    gate_pre = jnp.dot(normal, w_gate, preferred_element_type=jnp.float32).astype(jnp.bfloat16)
    up_pre = jnp.dot(normal, w_up, preferred_element_type=jnp.float32).astype(jnp.bfloat16)
    both = jnp.concatenate([gate_pre, up_pre], axis=1).astype(jnp.float32)
    taps = jnp.concatenate([conv_gate, conv_up], axis=1).astype(jnp.float32)
    total = both.shape[0]
    padded = jnp.concatenate([jnp.zeros((2, both.shape[1]), jnp.float32), both], axis=0)
    conv = taps[0] * padded[0:total] + taps[1] * padded[1:total + 1] + taps[2] * padded[2:total + 2]
    half = w_gate.shape[1]
    hidden = (jax.nn.silu(conv[:, :half]) * conv[:, half:]).astype(jnp.bfloat16)
    mixed = first + jnp.dot(hidden, w_down, preferred_element_type=jnp.float32)
    return mixed.astype(jnp.bfloat16)
```

```python
import functools

import jax
import jax.numpy as jnp
from jax import lax
from jax.experimental import pallas as pl
from jax.experimental.pallas import tpu as pltpu
from jax.sharding import PartitionSpec as P

EPS = 1e-06
NEG = -1e30


def from_behind(block, axis, distance):
    devices = range(lax.axis_size(axis))
    route = [(i - distance, i) for i in devices if i - distance in devices]
    return lax.ppermute(block, axis, route)


PLANE = 4


def gather_kernel(n, count, *refs):
    ins, outs = refs[:count], refs[count : 2 * count]
    local_sem, send_sem, recv_sem = refs[2 * count :]
    ring = n // PLANE
    reach = (ring - 1) // 2
    anti = ring // 2 if ring % 2 == 0 else 0
    me = lax.axis_index("sp")
    z, y, c = me // PLANE, lax.rem(me // 2, 2), lax.rem(me, 2)

    def place(dz, flip_y, flip_c):
        row = lax.rem(z + dz + ring, ring)
        col = 1 - y if flip_y else y
        core = 1 - c if flip_c else c
        return row * PLANE + col * 2 + core

    to = {"y": place(0, 1, 0), "up": place(1, 0, 0), "down": place(-1, 0, 0), "core": place(0, 0, 1)}

    events = {("own",): (0, 0, None), ("y",): (0, 1, None)}
    for other in (0, 1):
        for k in range(1, reach + 1):
            events[(other, "up", k)] = (-k, other, None)
            events[(other, "down", k)] = (k, other, None)
        if anti:
            events[(other, "anti", 0)] = (anti, other, 0)
            events[(other, "anti", 1)] = (anti, other, 1)
    keys = list(events)
    slots = {key: i for i, key in enumerate(keys)}
    slots.update({("core", key): len(keys) + i for i, key in enumerate(keys)})

    barrier = pltpu.get_barrier_semaphore()
    for target in to.values():
        pl.semaphore_signal(barrier, inc=1, device_id={"sp": target}, device_id_type=pl.DeviceIdType.MESH)
    pl.semaphore_wait(barrier, len(to))

    started = [[] for _ in range(count)]

    def part(ref, block, half):
        if half is None:
            return ref.at[block]
        rows = ref.shape[1] // 2
        return ref.at[block, pl.ds(half * rows, rows)]

    def copy_of(a, view, src, slot, target, number):
        return pltpu.make_async_remote_copy(
            src_ref=src,
            dst_ref=view,
            send_sem=send_sem.at[a, number],
            recv_sem=recv_sem.at[a, slot],
            device_id={"sp": target},
            device_id_type=pl.DeviceIdType.MESH,
        )

    def send(a, key, via, as_key, half=None):
        dz, other, own_half = events[key]
        half = own_half if half is None else half
        block = place(dz, other, 0)
        view = part(outs[a], block, half)
        src = ins[a] if key == ("own",) else view
        copy = copy_of(a, view, src, slots[as_key], to[via], len(started[a]))
        copy.start()
        started[a].append(copy)

    def arrived(a, key, from_core=False):
        dz, other, half = events[key]
        view = part(outs[a], place(dz, other, int(from_core)), half)
        slot = slots[("core", key)] if from_core else slots[key]
        copy_of(a, view, view, slot, to["core"], 0).wait_recv()

    def onward(a, key):
        other, way, k = key
        arrived(a, key)
        if way != "anti" and k < reach:
            send(a, key, way, (other, way, k + 1))
        elif way != "anti" and anti and not other:
            half = 0 if way == "up" else 1
            send(a, key, way, (other, "anti", half), half)
        elif way == "anti" and not other:
            send(a, key, "y", (1, "anti", k))
        send(a, key, "core", ("core", key))

    locals_ = []

    def stage0(a):
        copy = pltpu.make_async_copy(ins[a], outs[a].at[me], local_sem.at[a])
        copy.start()
        locals_.append(copy)
        send(a, ("own",), "y", ("y",))
        send(a, ("own",), "up", (0, "up", 1))
        send(a, ("own",), "down", (0, "down", 1))
        send(a, ("own",), "core", ("core", ("own",)))

    def stage1(a):
        arrived(a, ("y",))
        send(a, ("y",), "up", (1, "up", 1))
        send(a, ("y",), "down", (1, "down", 1))
        send(a, ("y",), "core", ("core", ("y",)))
        for k in range(1, reach + 1):
            onward(a, (0, "up", k))
            onward(a, (0, "down", k))

    def stage2(a):
        if anti:
            onward(a, (0, "anti", 0))
            onward(a, (0, "anti", 1))
        for k in range(1, reach + 1):
            onward(a, (1, "up", k))
            onward(a, (1, "down", k))

    def stage3(a):
        if anti:
            onward(a, (1, "anti", 0))
            onward(a, (1, "anti", 1))

    def stage4(a):
        for key in keys:
            arrived(a, key, from_core=True)

    stage0(0)
    for tick in range(1, count + 6):
        for lag, stage in enumerate((stage0, None, stage1, stage2, stage3, stage4)):
            a = tick - lag
            if stage is not None and 0 <= a < count and not (stage is stage0 and a == 0):
                stage(a)
    for a in range(count):
        locals_[a].wait()
        for copy in started[a]:
            copy.wait_send()


def gather_all(arrays):
    n = lax.axis_size("sp")
    ring = n // PLANE
    if n % PLANE or ring < 3:
        return [lax.all_gather(x, "sp", axis=0) for x in arrays]
    count = len(arrays)
    return pl.pallas_call(
        functools.partial(gather_kernel, n, count),
        out_shape=[jax.ShapeDtypeStruct((n,) + x.shape, x.dtype) for x in arrays],
        in_specs=[pl.BlockSpec(memory_space=pltpu.VMEM)] * count,
        out_specs=[pl.BlockSpec(memory_space=pl.ANY)] * count,
        scratch_shapes=[
            pltpu.SemaphoreType.DMA((count,)),
            pltpu.SemaphoreType.DMA((count, n // 2 * 3)),
            pltpu.SemaphoreType.DMA((count, n + 8)),
        ],
        compiler_params=pltpu.CompilerParams(collective_id=0, has_side_effects=True),
    )(*arrays)


def globalize(part, rows):
    heads = part.shape[1]
    blocks = part.reshape(-1, rows, heads)
    totals = blocks[:, -1, :]
    before = jnp.cumsum(totals, axis=0) - totals
    return (blocks + before[:, None, :]).reshape(part.shape)


def attend(carry, keys, values, queries, cum_own, cum_every, qpos):
    top, denom, accum = carry
    count = keys.shape[0]
    heads = queries.shape[1]
    size = queries.shape[2]
    keys = keys.reshape(count, heads, size)
    values = values.reshape(count, heads, size)
    kpos = jnp.arange(count, dtype=jnp.int32)
    scores = jnp.einsum(
        "qhd,khd->qhk", queries, keys, preferred_element_type=jnp.float32
    ) * size ** (-0.5)
    scores = scores + cum_own[:, :, None] - cum_every.T[None, :, :]
    keep = (kpos[None, :] <= qpos[:, None])[:, None, :]
    scores = jnp.where(keep, scores, NEG)
    new_top = jnp.maximum(top, jnp.max(scores, axis=-1))
    weights = jnp.where(keep, jnp.exp(scores - new_top[:, :, None]), 0.0)
    denom = jnp.sum(weights, axis=-1)
    accum = jnp.einsum(
        "qhk,khd->qhd", weights.astype(jnp.bfloat16), values, preferred_element_type=jnp.float32
    )
    return (new_top, denom, accum)


def finish(carry):
    top, denom, accum = carry
    attended = accum / denom[:, :, None]
    normed = attended * lax.rsqrt(jnp.mean(attended * attended, axis=-1, keepdims=True) + EPS)
    return normed.astype(jnp.bfloat16).reshape(attended.shape[0], -1)


def empty_carry(rows, heads, size):
    return (
        jnp.full((rows, heads), NEG, jnp.float32),
        jnp.zeros((rows, heads), jnp.float32),
        jnp.zeros((rows, heads, size), jnp.float32),
    )


def body(
    residual,
    q_small,
    k_small,
    v_small,
    q_large,
    k_large,
    v_large,
    forget_small,
    forget_large,
    w_out_small,
    w_out_large,
    norm_gain,
    w_gate,
    w_up,
    conv_gate,
    conv_up,
    w_down,
):
    rows = q_small.shape[0]
    offset = lax.axis_index("sp") * rows
    qpos = offset + jnp.arange(rows, dtype=jnp.int32)
    local_small = jnp.cumsum(jax.nn.log_sigmoid(forget_small), axis=0)
    local_large = jnp.cumsum(jax.nn.log_sigmoid(forget_large), axis=0)
    heads_small = forget_small.shape[1]
    heads_large = forget_large.shape[1]
    local = jnp.concatenate([local_small, local_large], axis=1).T
    padded = jnp.pad(local, ((0, -local.shape[0] % 16), (0, 0)))
    every, keys_s, values_s, keys_l, values_l, gate_full, up_full, down_blocks = gather_all(
        [padded, k_small, v_small, k_large, v_large, w_gate, w_up, w_down]
    )
    flat = lambda x: x.reshape(-1, x.shape[-1])
    keys_s, values_s, keys_l, values_l = map(flat, (keys_s, values_s, keys_l, values_l))
    gate_full, up_full = flat(gate_full), flat(up_full)
    part = every.transpose(0, 2, 1).reshape(-1, padded.shape[0])
    every_small = globalize(part[:, :heads_small], rows)
    every_large = globalize(part[:, heads_small : heads_small + heads_large], rows)
    cum_small = lax.dynamic_slice_in_dim(every_small, offset, rows, 0)
    cum_large = lax.dynamic_slice_in_dim(every_large, offset, rows, 0)
    queries_small = q_small.reshape(rows, heads_small, -1)
    queries_large = q_large.reshape(rows, heads_large, -1)
    start_carry = (
        empty_carry(rows, heads_small, queries_small.shape[2]),
        empty_carry(rows, heads_large, queries_large.shape[2]),
    )
    small = attend(start_carry[0], keys_s, values_s, queries_small, cum_small, every_small, qpos)
    large = attend(start_carry[1], keys_l, values_l, queries_large, cum_large, every_large, qpos)
    normed_small = finish(small)
    normed_large = finish(large)
    first_part = jnp.dot(normed_small, w_out_small, preferred_element_type=jnp.float32)
    projected = lax.psum_scatter(
        (
            first_part + jnp.dot(normed_large, w_out_large, preferred_element_type=jnp.float32)
        ).astype(jnp.bfloat16),
        "tp",
        scatter_dimension=0,
        tiled=True,
    ).astype(jnp.float32)
    first = residual.astype(jnp.float32) + projected
    normal = (
        first * lax.rsqrt(jnp.mean(first * first, axis=-1, keepdims=True) + EPS) * norm_gain
    ).astype(jnp.bfloat16)
    piece = lax.all_gather(normal, "tp", axis=0, tiled=True)
    gate_part = jnp.dot(piece, gate_full, preferred_element_type=jnp.float32).astype(jnp.bfloat16)
    up_part = jnp.dot(piece, up_full, preferred_element_type=jnp.float32).astype(jnp.bfloat16)
    both = jnp.concatenate([gate_part, up_part], axis=1)
    width = both.shape[0]
    rim = from_behind(both[width - 2 :], "sp", 1)
    extended = jnp.concatenate([rim, both], axis=0).astype(jnp.float32)
    taps = jnp.concatenate([conv_gate, conv_up], axis=1)
    conv = (
        taps[0] * extended[0:width]
        + taps[1] * extended[1 : width + 1]
        + taps[2] * extended[2 : width + 2]
    )
    half = gate_full.shape[1]
    hidden = (jax.nn.silu(conv[:, :half]) * conv[:, half:]).astype(jnp.bfloat16)
    mixed = first + lax.psum_scatter(
        jnp.einsum("th,nhc->tnc", hidden, down_blocks, preferred_element_type=jnp.float32)
        .astype(jnp.bfloat16)
        .reshape(width, -1),
        "tp",
        scatter_dimension=0,
        tiled=True,
    ).astype(jnp.float32)
    return mixed.astype(jnp.bfloat16)


def solution(mesh):
    placed = (
        P(("sp", "tp"), None),
        P("sp", "tp"),
        P("sp", "tp"),
        P("sp", "tp"),
        P("sp", "tp"),
        P("sp", "tp"),
        P("sp", "tp"),
        P("sp", "tp"),
        P("sp", "tp"),
        P("tp", None),
        P("tp", None),
        P(),
        P("sp", "tp"),
        P("sp", "tp"),
        P(None, "tp"),
        P(None, "tp"),
        P("tp", "sp"),
    )
    return jax.shard_map(
        body, mesh=mesh, in_specs=placed, out_specs=P(("sp", "tp"), None), check_vma=False
    )
```

```python
import functools

import jax
import jax.numpy as jnp
from jax import lax
from jax.experimental import pallas as pl
from jax.experimental.pallas import tpu as pltpu
from jax.sharding import PartitionSpec as P

EPS = 1e-06
NEG = -1e30


def from_behind(block, axis, distance):
    devices = range(lax.axis_size(axis))
    route = [(i - distance, i) for i in devices if i - distance in devices]
    return lax.ppermute(block, axis, route)


PLANE = 4
PIECE = 1 << 18
UP, DOWN, UP_OTHER, DOWN_OTHER, ACROSS, CORE, CORE_OTHER = range(7)
OWN, OTHER = 0, 1
MESH = pl.DeviceIdType.MESH


def gather_kernel(n, count, items, *refs):
    ins, outs = refs[:count], refs[count : 2 * count]
    local_sem, send_sem, recv_sem = refs[2 * count :]
    line = n // PLANE
    me = lax.axis_index("sp")
    z, y, c = me // PLANE, lax.rem(me // 2, 2), lax.rem(me, 2)

    def place(row, flip_y, flip_c):
        return row * PLANE + (1 - y if flip_y else y) * 2 + (1 - c if flip_c else c)

    across, core = place(z, 1, 0), place(z, 0, 1)
    above, below = place(jnp.minimum(z + 1, line - 1), 0, 0), place(jnp.maximum(z - 1, 0), 0, 0)
    barrier = pltpu.get_barrier_semaphore()

    def greet(target):
        pl.semaphore_signal(barrier, inc=1, device_id={"sp": target}, device_id_type=MESH)

    greet(across)
    greet(core)
    pl.when(z < line - 1)(lambda: greet(above))
    pl.when(z > 0)(lambda: greet(below))
    pl.semaphore_wait(barrier, 2 + jnp.minimum(z, 1) + jnp.minimum(line - 1 - z, 1))

    def view(i, row, other, other_core=0):
        a, start, size, _ = items[i]
        return outs[a].at[place(row, other, other_core), pl.ds(start, size)]

    def copy_of(i, src, dst, via, row, slot, target):
        return pltpu.make_async_remote_copy(
            src_ref=src,
            dst_ref=dst,
            send_sem=send_sem.at[i, via, row],
            recv_sem=recv_sem.at[i, slot, row],
            device_id={"sp": target},
            device_id_type=MESH,
        )

    def send(i, via, row, other, first=False):
        dst = view(i, row, other)
        a, start, size, _ = items[i]
        src = ins[a].at[pl.ds(start, size)] if first else dst
        target = {UP: above, UP_OTHER: above, DOWN: below, DOWN_OTHER: below, ACROSS: across}.get(via, core)
        slot = {ACROSS: OTHER, CORE: 2 + OWN, CORE_OTHER: 2 + OTHER}.get(via, other)
        return copy_of(i, src, dst, via, row, slot, target)

    def arrived(i, row, other):
        copy_of(i, view(i, row, other), view(i, row, other), CORE, row, other, core).wait_recv()

    def on_z(i, other, k, act, kinds):
        up, down = (UP_OTHER, DOWN_OTHER) if other else (UP, DOWN)

        @pl.when(z - k >= 0)
        def _():
            if "wait" in kinds:
                arrived(i, z - k, other)
            pl.when(z < line - 1)(lambda: act(send(i, up, z - k, other)))
            onward(i, z - k, other, act)

        @pl.when(z + k <= line - 1)
        def _():
            if "wait" in kinds:
                arrived(i, z + k, other)
            pl.when(z > 0)(lambda: act(send(i, down, z + k, other)))
            onward(i, z + k, other, act)

    def onward(i, row, other, act):
        if not other and not items[i][3]:
            act(send(i, ACROSS, row, 0))
        act(send(i, CORE_OTHER if other else CORE, row, other))

    start = lambda copy: copy.start()
    finish_send = lambda copy: copy.wait_send()

    def local(i):
        a, first, size, _ = items[i]
        return pltpu.make_async_copy(ins[a].at[pl.ds(first, size)], view(i, z, 0), local_sem.at[i])

    def stage_own(i, act):
        pl.when(z < line - 1)(lambda: act(send(i, UP, z, 0, True)))
        pl.when(z > 0)(lambda: act(send(i, DOWN, z, 0, True)))
        act(send(i, ACROSS, z, 0, True))
        act(send(i, CORE, z, 0, True))

    def stage_column(i, act, kinds):
        if "wait" in kinds:
            arrived(i, z, 1)
        pl.when(z < line - 1)(lambda: act(send(i, UP_OTHER, z, 1)))
        pl.when(z > 0)(lambda: act(send(i, DOWN_OTHER, z, 1)))
        act(send(i, CORE_OTHER, z, 1))

    def stage(i, k, act, kinds):
        early = items[i][3]
        if k == 0:
            if "wait" in kinds:
                local(i).start()
            stage_own(i, act)
        elif k < line:
            on_z(i, 0, k, act, kinds)
        if early and k == 1:
            stage_column(i, act, kinds)
        if early and 2 <= k <= line:
            on_z(i, 1, k - 1, act, kinds)
        if not early and k == line:
            for row in range(line):
                if "wait" in kinds:
                    arrived(i, row, 1)
                act(send(i, CORE_OTHER, row, 1))
        if k == line + 1 and "wait" in kinds:
            for row in range(line):
                for other in (0, 1):
                    dst = view(i, row, other, 1)
                    copy_of(i, dst, dst, CORE, row, 2 + other, core).wait_recv()

    total = len(items)
    stage(0, 0, start, ("wait",))
    stage(1, 0, start, ("wait",))
    for tick in range(1, total + line + 2):
        if 1 < tick + 1 < total:
            stage(tick + 1, 0, start, ("wait",))
        for k in range(1, line + 2):
            if 0 <= tick - k < total:
                stage(tick - k, k, start, ("wait",))
    for i in range(total):
        local(i).wait()
        for k in range(line + 1):
            stage(i, k, finish_send, ())


def gather_all(arrays, early):
    n = lax.axis_size("sp")
    line = n // PLANE
    if n % PLANE or line < 2:
        return [lax.all_gather(x, "sp", axis=0) for x in arrays]
    count = len(arrays)
    items = []
    for a, x in enumerate(arrays):
        rows = x.shape[0]
        pieces = max(1, x.size * x.dtype.itemsize // PIECE)
        while rows % (16 * pieces) and pieces > 1:
            pieces -= 1
        items += [(a, j * (rows // pieces), rows // pieces, early[a]) for j in range(pieces)]
    total = len(items)
    return pl.pallas_call(
        functools.partial(gather_kernel, n, count, items),
        out_shape=[jax.ShapeDtypeStruct((n,) + x.shape, x.dtype) for x in arrays],
        in_specs=[pl.BlockSpec(memory_space=pltpu.VMEM)] * count,
        out_specs=[pl.BlockSpec(memory_space=pl.ANY)] * count,
        scratch_shapes=[
            pltpu.SemaphoreType.DMA((total,)),
            pltpu.SemaphoreType.DMA((total, 7, line)),
            pltpu.SemaphoreType.DMA((total, 4, line)),
        ],
        compiler_params=pltpu.CompilerParams(collective_id=0, has_side_effects=True),
    )(*arrays)


def attention_kernel(rows, per, size_s, size_l, cum, q_s, k_s, v_s, q_l, k_l, v_l, out_s, out_l):
    offset = pl.multiple_of(lax.axis_index("sp") * rows, rows)
    own = cum[:, pl.ds(offset, rows)].T
    keep = None

    def head(q, k_ref, v_ref, row, size):
        lanes = k_ref.shape[-1]
        keys = k_ref[...].reshape(-1, lanes)
        values = v_ref[...].reshape(-1, lanes)
        nonlocal keep
        if keep is None:
            shape = (rows, keys.shape[0])
            keep = lax.broadcasted_iota(jnp.int32, shape, 1) <= offset + lax.broadcasted_iota(
                jnp.int32, shape, 0
            )
        scores = lax.dot_general(
            q, keys, (((1,), (1,)), ((), ())), preferred_element_type=jnp.float32
        ) * size ** (-0.5)
        scores = scores + own[:, row : row + 1] - cum[row : row + 1, :]
        scores = jnp.where(keep, scores, NEG)
        weights = jnp.exp(scores - jnp.max(scores, axis=-1, keepdims=True))
        denom = jnp.sum(weights, axis=-1, keepdims=True)
        accum = jnp.dot(weights.astype(jnp.bfloat16), values, preferred_element_type=jnp.float32)
        return accum / denom

    attended = head(q_l[...], k_l, v_l, per, size_l)
    mean = jnp.mean(attended * attended, axis=-1, keepdims=True)
    out_l[...] = (attended * lax.rsqrt(mean + EPS)).astype(jnp.bfloat16)
    q = q_s[...]
    lane = lax.broadcasted_iota(jnp.int32, q.shape, 1)
    normed = jnp.zeros(q.shape, jnp.float32)
    for h in range(per):
        mine = (lane >= h * size_s) & (lane < (h + 1) * size_s)
        attended = head(jnp.where(mine, q, jnp.zeros_like(q)), k_s, v_s, h, size_s)
        attended = jnp.where(mine, attended, 0.0)
        mean = jnp.sum(attended * attended, axis=-1, keepdims=True) / size_s
        normed = normed + attended * lax.rsqrt(mean + EPS)
    out_s[...] = normed.astype(jnp.bfloat16)


def attention(cum, steps, per, q_s, k_s, v_s, q_l, k_l, v_l):
    n, rows = k_s.shape[0], q_s.shape[0]
    wide_s, wide_l = q_s.shape[1] // steps, q_l.shape[1] // steps
    of_q = lambda wide: pl.BlockSpec((rows, wide), lambda s: (0, s))
    of_k = lambda wide: pl.BlockSpec((n, k_s.shape[1], wide), lambda s: (0, 0, s))
    return pl.pallas_call(
        functools.partial(attention_kernel, rows, per, wide_s // per, wide_l),
        grid=(steps,),
        in_specs=[pl.BlockSpec((8, cum.shape[1]), lambda s: (s, 0))]
        + [of_q(wide_s), of_k(wide_s), of_k(wide_s), of_q(wide_l), of_k(wide_l), of_k(wide_l)],
        out_specs=[of_q(wide_s), of_q(wide_l)],
        out_shape=[
            jax.ShapeDtypeStruct(q_s.shape, jnp.bfloat16),
            jax.ShapeDtypeStruct(q_l.shape, jnp.bfloat16),
        ],
    )(cum, q_s, k_s, v_s, q_l, k_l, v_l)


def down_kernel(hidden, block, out):
    out[...] = jnp.dot(hidden[...], block[0], preferred_element_type=jnp.float32).astype(out.dtype)


def down_product(hidden, blocks):
    n, depth, wide = blocks.shape
    rows = hidden.shape[0]
    if wide % 128:
        full = jnp.einsum("th,nhc->tnc", hidden, blocks, preferred_element_type=jnp.float32)
        return full.astype(jnp.bfloat16).reshape(rows, -1)
    return pl.pallas_call(
        down_kernel,
        grid=(n,),
        in_specs=[
            pl.BlockSpec((rows, depth), lambda i: (0, 0)),
            pl.BlockSpec((1, depth, wide), lambda i: (i, 0, 0)),
        ],
        out_specs=pl.BlockSpec((rows, wide), lambda i: (0, i)),
        out_shape=jax.ShapeDtypeStruct((rows, n * wide), jnp.bfloat16),
    )(hidden, blocks)


def body(
    residual,
    q_small,
    k_small,
    v_small,
    q_large,
    k_large,
    v_large,
    forget_small,
    forget_large,
    w_out_small,
    w_out_large,
    norm_gain,
    w_gate,
    w_up,
    conv_gate,
    conv_up,
    w_down,
):
    steps = forget_large.shape[1]
    per = forget_small.shape[1] // steps
    rows = q_small.shape[0]
    local_small = jnp.cumsum(jax.nn.log_sigmoid(forget_small), axis=0)
    local_large = jnp.cumsum(jax.nn.log_sigmoid(forget_large), axis=0)
    local = jnp.concatenate(
        [
            local_small.T.reshape(steps, per, rows),
            local_large.T.reshape(steps, 1, rows),
            jnp.zeros((steps, 7 - per, rows), jnp.float32),
        ],
        axis=1,
    ).reshape(steps * 8, rows)
    every, keys_s, values_s, keys_l, values_l, gate_full, up_full, down_blocks = gather_all(
        [local, k_small, v_small, k_large, v_large, w_gate, w_up, w_down],
        [False, True, True, True, False, False, False, False],
    )
    flat = lambda x: x.reshape(-1, x.shape[-1])
    gate_full, up_full = flat(gate_full), flat(up_full)
    totals = every[:, :, -1]
    before = jnp.cumsum(totals, axis=0) - totals
    cum = (every + before[:, :, None]).transpose(1, 0, 2).reshape(steps * 8, -1)
    normed_small, normed_large = attention(
        cum, steps, per, q_small, keys_s, values_s, q_large, keys_l, values_l
    )
    first_part = jnp.dot(normed_small, w_out_small, preferred_element_type=jnp.float32)
    projected = lax.psum_scatter(
        (
            first_part + jnp.dot(normed_large, w_out_large, preferred_element_type=jnp.float32)
        ).astype(jnp.bfloat16),
        "tp",
        scatter_dimension=0,
        tiled=True,
    ).astype(jnp.float32)
    first = residual.astype(jnp.float32) + projected
    normal = (
        first * lax.rsqrt(jnp.mean(first * first, axis=-1, keepdims=True) + EPS) * norm_gain
    ).astype(jnp.bfloat16)
    piece = lax.all_gather(normal, "tp", axis=0, tiled=True)
    gate_part = jnp.dot(piece, gate_full, preferred_element_type=jnp.float32).astype(jnp.bfloat16)
    up_part = jnp.dot(piece, up_full, preferred_element_type=jnp.float32).astype(jnp.bfloat16)
    both = jnp.concatenate([gate_part, up_part], axis=1)
    width = both.shape[0]
    rim = from_behind(both[width - 2 :], "sp", 1)
    extended = jnp.concatenate([rim, both], axis=0).astype(jnp.float32)
    taps = jnp.concatenate([conv_gate, conv_up], axis=1)
    conv = (
        taps[0] * extended[0:width]
        + taps[1] * extended[1 : width + 1]
        + taps[2] * extended[2 : width + 2]
    )
    half = gate_full.shape[1]
    hidden = (jax.nn.silu(conv[:, :half]) * conv[:, half:]).astype(jnp.bfloat16)
    mixed = first + lax.psum_scatter(
        down_product(hidden, down_blocks),
        "tp",
        scatter_dimension=0,
        tiled=True,
    ).astype(jnp.float32)
    return mixed.astype(jnp.bfloat16)


def solution(mesh):
    placed = (
        P(("sp", "tp"), None),
        P("sp", "tp"),
        P("sp", "tp"),
        P("sp", "tp"),
        P("sp", "tp"),
        P("sp", "tp"),
        P("sp", "tp"),
        P("sp", "tp"),
        P("sp", "tp"),
        P("tp", None),
        P("tp", None),
        P(),
        P("sp", "tp"),
        P("sp", "tp"),
        P(None, "tp"),
        P(None, "tp"),
        P("tp", "sp"),
    )
    return jax.shard_map(
        body, mesh=mesh, in_specs=placed, out_specs=P(("sp", "tp"), None), check_vma=False
    )
```

```python
import functools

import jax
import jax.numpy as jnp
from jax import lax
from jax.experimental import pallas as pl
from jax.experimental.pallas import tpu as pltpu
from jax.sharding import PartitionSpec as P

EPS = 1e-06
NEG = -1e30


def from_behind(block, axis, distance):
    devices = range(lax.axis_size(axis))
    route = [(i - distance, i) for i in devices if i - distance in devices]
    return lax.ppermute(block, axis, route)


PLANE = 4
PIECE = 1 << 17
UP, DOWN, UP_OTHER, DOWN_OTHER, ACROSS, CORE, CORE_OTHER = range(7)
OWN, OTHER = 0, 1
MESH = pl.DeviceIdType.MESH


def gather_kernel(n, count, items, *refs):
    ins, outs = refs[:count], refs[count : 2 * count]
    local_sem, send_sem, recv_sem = refs[2 * count :]
    line = n // PLANE
    me = lax.axis_index("sp")
    z, y, c = me // PLANE, lax.rem(me // 2, 2), lax.rem(me, 2)

    def place(row, flip_y, flip_c):
        return row * PLANE + (1 - y if flip_y else y) * 2 + (1 - c if flip_c else c)

    across, core = place(z, 1, 0), place(z, 0, 1)
    above, below = place(jnp.minimum(z + 1, line - 1), 0, 0), place(jnp.maximum(z - 1, 0), 0, 0)
    barrier = pltpu.get_barrier_semaphore()

    def greet(target):
        pl.semaphore_signal(barrier, inc=1, device_id={"sp": target}, device_id_type=MESH)

    greet(across)
    greet(core)
    pl.when(z < line - 1)(lambda: greet(above))
    pl.when(z > 0)(lambda: greet(below))
    pl.semaphore_wait(barrier, 2 + jnp.minimum(z, 1) + jnp.minimum(line - 1 - z, 1))

    def view(i, row, other, other_core=0):
        a, start, size, _ = items[i]
        return outs[a].at[place(row, other, other_core), pl.ds(start, size)]

    def copy_of(i, src, dst, via, row, slot, target):
        return pltpu.make_async_remote_copy(
            src_ref=src,
            dst_ref=dst,
            send_sem=send_sem.at[i, via, row],
            recv_sem=recv_sem.at[i, slot, row],
            device_id={"sp": target},
            device_id_type=MESH,
        )

    def send(i, via, row, other, first=False):
        dst = view(i, row, other)
        a, start, size, _ = items[i]
        src = ins[a].at[pl.ds(start, size)] if first else dst
        target = {UP: above, UP_OTHER: above, DOWN: below, DOWN_OTHER: below, ACROSS: across}.get(via, core)
        slot = {ACROSS: OTHER, CORE: 2 + OWN, CORE_OTHER: 2 + OTHER}.get(via, other)
        return copy_of(i, src, dst, via, row, slot, target)

    def arrived(i, row, other):
        copy_of(i, view(i, row, other), view(i, row, other), CORE, row, other, core).wait_recv()

    def on_z(i, other, k, act, kinds):
        up, down = (UP_OTHER, DOWN_OTHER) if other else (UP, DOWN)

        @pl.when(z - k >= 0)
        def _():
            if "wait" in kinds:
                arrived(i, z - k, other)
            pl.when(z < line - 1)(lambda: act(send(i, up, z - k, other)))
            onward(i, z - k, other, act)

        @pl.when(z + k <= line - 1)
        def _():
            if "wait" in kinds:
                arrived(i, z + k, other)
            pl.when(z > 0)(lambda: act(send(i, down, z + k, other)))
            onward(i, z + k, other, act)

    def onward(i, row, other, act):
        if not other and not items[i][3]:
            act(send(i, ACROSS, row, 0))
        act(send(i, CORE_OTHER if other else CORE, row, other))

    start = lambda copy: copy.start()
    finish_send = lambda copy: copy.wait_send()

    def local(i):
        a, first, size, _ = items[i]
        return pltpu.make_async_copy(ins[a].at[pl.ds(first, size)], view(i, z, 0), local_sem.at[i])

    def stage_own(i, act):
        pl.when(z < line - 1)(lambda: act(send(i, UP, z, 0, True)))
        pl.when(z > 0)(lambda: act(send(i, DOWN, z, 0, True)))
        act(send(i, ACROSS, z, 0, True))
        act(send(i, CORE, z, 0, True))

    def stage_column(i, act, kinds):
        if "wait" in kinds:
            arrived(i, z, 1)
        pl.when(z < line - 1)(lambda: act(send(i, UP_OTHER, z, 1)))
        pl.when(z > 0)(lambda: act(send(i, DOWN_OTHER, z, 1)))
        act(send(i, CORE_OTHER, z, 1))

    def stage(i, k, act, kinds):
        early = items[i][3]
        if k == 0:
            if "wait" in kinds:
                local(i).start()
            stage_own(i, act)
        elif k < line:
            on_z(i, 0, k, act, kinds)
        if early and k == 1:
            stage_column(i, act, kinds)
        if early and 2 <= k <= line:
            on_z(i, 1, k - 1, act, kinds)
        if not early and k == line:
            for row in range(line):
                if "wait" in kinds:
                    arrived(i, row, 1)
                act(send(i, CORE_OTHER, row, 1))
        if k == line + 1 and "wait" in kinds:
            for row in range(line):
                for other in (0, 1):
                    dst = view(i, row, other, 1)
                    copy_of(i, dst, dst, CORE, row, 2 + other, core).wait_recv()

    total = len(items)
    stage(0, 0, start, ("wait",))
    stage(1, 0, start, ("wait",))
    for tick in range(1, total + line + 2):
        if 1 < tick + 1 < total:
            stage(tick + 1, 0, start, ("wait",))
        for k in range(1, line + 2):
            if 0 <= tick - k < total:
                stage(tick - k, k, start, ("wait",))
    for i in range(total):
        local(i).wait()
        for k in range(line + 1):
            stage(i, k, finish_send, ())


def gather_all(arrays, early):
    n = lax.axis_size("sp")
    line = n // PLANE
    if n % PLANE or line < 2:
        return [lax.all_gather(x, "sp", axis=0) for x in arrays]
    count = len(arrays)
    items = []
    for a, x in enumerate(arrays):
        rows = x.shape[0]
        pieces = max(1, x.size * x.dtype.itemsize // PIECE)
        while rows % (16 * pieces) and pieces > 1:
            pieces -= 1
        items += [(a, j * (rows // pieces), rows // pieces, early[a]) for j in range(pieces)]
    total = len(items)
    return pl.pallas_call(
        functools.partial(gather_kernel, n, count, items),
        out_shape=[jax.ShapeDtypeStruct((n,) + x.shape, x.dtype) for x in arrays],
        in_specs=[pl.BlockSpec(memory_space=pltpu.VMEM)] * count,
        out_specs=[pl.BlockSpec(memory_space=pl.ANY)] * count,
        scratch_shapes=[
            pltpu.SemaphoreType.DMA((total,)),
            pltpu.SemaphoreType.DMA((total, 7, line)),
            pltpu.SemaphoreType.DMA((total, 4, line)),
        ],
        compiler_params=pltpu.CompilerParams(collective_id=0, has_side_effects=True),
    )(*arrays)


def attention_kernel(rows, per, size_s, size_l, cum, q_s, k_s, v_s, q_l, k_l, v_l, out_s, out_l):
    offset = pl.multiple_of(lax.axis_index("sp") * rows, rows)
    own = cum[:, pl.ds(offset, rows)].T
    keep = None

    def head(q, k_ref, v_ref, row, size):
        lanes = k_ref.shape[-1]
        keys = k_ref[...].reshape(-1, lanes)
        values = v_ref[...].reshape(-1, lanes)
        nonlocal keep
        if keep is None:
            shape = (rows, keys.shape[0])
            keep = lax.broadcasted_iota(jnp.int32, shape, 1) <= offset + lax.broadcasted_iota(
                jnp.int32, shape, 0
            )
        scores = lax.dot_general(
            q, keys, (((1,), (1,)), ((), ())), preferred_element_type=jnp.float32
        ) * size ** (-0.5)
        scores = scores + own[:, row : row + 1] - cum[row : row + 1, :]
        scores = jnp.where(keep, scores, NEG)
        weights = jnp.exp(scores - jnp.max(scores, axis=-1, keepdims=True))
        denom = jnp.sum(weights, axis=-1, keepdims=True)
        accum = jnp.dot(weights.astype(jnp.bfloat16), values, preferred_element_type=jnp.float32)
        return accum / denom

    attended = head(q_l[...], k_l, v_l, per, size_l)
    mean = jnp.mean(attended * attended, axis=-1, keepdims=True)
    out_l[...] = (attended * lax.rsqrt(mean + EPS)).astype(jnp.bfloat16)
    q = q_s[...]
    lane = lax.broadcasted_iota(jnp.int32, q.shape, 1)
    normed = jnp.zeros(q.shape, jnp.float32)
    for h in range(per):
        mine = (lane >= h * size_s) & (lane < (h + 1) * size_s)
        attended = head(jnp.where(mine, q, jnp.zeros_like(q)), k_s, v_s, h, size_s)
        attended = jnp.where(mine, attended, 0.0)
        mean = jnp.sum(attended * attended, axis=-1, keepdims=True) / size_s
        normed = normed + attended * lax.rsqrt(mean + EPS)
    out_s[...] = normed.astype(jnp.bfloat16)


def attention(cum, steps, per, q_s, k_s, v_s, q_l, k_l, v_l):
    n, rows = k_s.shape[0], q_s.shape[0]
    wide_s, wide_l = q_s.shape[1] // steps, q_l.shape[1] // steps
    of_q = lambda wide: pl.BlockSpec((rows, wide), lambda s: (0, s))
    of_k = lambda wide: pl.BlockSpec((n, k_s.shape[1], wide), lambda s: (0, 0, s))
    return pl.pallas_call(
        functools.partial(attention_kernel, rows, per, wide_s // per, wide_l),
        grid=(steps,),
        in_specs=[pl.BlockSpec((8, cum.shape[1]), lambda s: (s, 0))]
        + [of_q(wide_s), of_k(wide_s), of_k(wide_s), of_q(wide_l), of_k(wide_l), of_k(wide_l)],
        out_specs=[of_q(wide_s), of_q(wide_l)],
        out_shape=[
            jax.ShapeDtypeStruct(q_s.shape, jnp.bfloat16),
            jax.ShapeDtypeStruct(q_l.shape, jnp.bfloat16),
        ],
    )(cum, q_s, k_s, v_s, q_l, k_l, v_l)


def exchange_kernel(n, spread, x, out, local_sem, send_sem, recv_sem):
    me = lax.axis_index("tp")
    barrier = pltpu.get_barrier_semaphore()
    for d in range(1, n):
        pl.semaphore_signal(barrier, inc=1, device_id={"tp": lax.rem(me + d, n)}, device_id_type=MESH)
    pl.semaphore_wait(barrier, n - 1)
    copies = []
    for d in range(1, n):
        target = lax.rem(me + d, n)
        copy = pltpu.make_async_remote_copy(
            src_ref=x.at[target] if spread else x,
            dst_ref=out.at[me],
            send_sem=send_sem.at[d],
            recv_sem=recv_sem.at[d],
            device_id={"tp": target},
            device_id_type=MESH,
        )
        copy.start()
        copies.append(copy)
    local = pltpu.make_async_copy(x.at[me] if spread else x, out.at[me], local_sem)
    local.start()
    for d in range(1, n):
        view = out.at[lax.rem(me - d + n, n)]
        pltpu.make_async_remote_copy(
            src_ref=view,
            dst_ref=view,
            send_sem=send_sem.at[d],
            recv_sem=recv_sem.at[d],
            device_id={"tp": lax.rem(me + d, n)},
            device_id_type=MESH,
        ).wait_recv()
    for copy in copies:
        copy.wait_send()
    local.wait()


def exchange(x, spread, number):
    n = lax.axis_size("tp")
    block = x.shape[1:] if spread else x.shape
    if n == 1:
        return x if spread else x[None]
    return pl.pallas_call(
        functools.partial(exchange_kernel, n, spread),
        out_shape=jax.ShapeDtypeStruct((n,) + block, x.dtype),
        in_specs=[pl.BlockSpec(memory_space=pltpu.VMEM)],
        out_specs=pl.BlockSpec(memory_space=pltpu.VMEM),
        scratch_shapes=[
            pltpu.SemaphoreType.DMA,
            pltpu.SemaphoreType.DMA((n,)),
            pltpu.SemaphoreType.DMA((n,)),
        ],
        compiler_params=pltpu.CompilerParams(collective_id=number, has_side_effects=True),
    )(x)


def sum_over_tp(part, number):
    n = lax.axis_size("tp")
    parts = exchange(part.astype(jnp.bfloat16).reshape(n, -1, part.shape[-1]), True, number)
    return jnp.sum(parts.astype(jnp.float32), axis=0)


def down_kernel(hidden, blocks, out):
    wide = jnp.concatenate([blocks[i] for i in range(blocks.shape[0])], axis=1)
    out[...] = jnp.dot(hidden[...], wide, preferred_element_type=jnp.float32).astype(out.dtype)


def down_product(hidden, blocks):
    n, depth, wide = blocks.shape
    rows = hidden.shape[0]
    if wide % 128:
        full = jnp.einsum("th,nhc->tnc", hidden, blocks, preferred_element_type=jnp.float32)
        return full.astype(jnp.bfloat16).reshape(rows, -1)
    fan = 4 if n % 4 == 0 else 1
    return pl.pallas_call(
        down_kernel,
        grid=(n // fan,),
        in_specs=[
            pl.BlockSpec((rows, depth), lambda i: (0, 0)),
            pl.BlockSpec((fan, depth, wide), lambda i: (i, 0, 0)),
        ],
        out_specs=pl.BlockSpec((rows, fan * wide), lambda i: (0, i)),
        out_shape=jax.ShapeDtypeStruct((rows, n * wide), jnp.bfloat16),
    )(hidden, blocks)


def body(
    residual,
    q_small,
    k_small,
    v_small,
    q_large,
    k_large,
    v_large,
    forget_small,
    forget_large,
    w_out_small,
    w_out_large,
    norm_gain,
    w_gate,
    w_up,
    conv_gate,
    conv_up,
    w_down,
):
    steps = forget_large.shape[1]
    per = forget_small.shape[1] // steps
    rows = q_small.shape[0]
    local_small = jnp.cumsum(jax.nn.log_sigmoid(forget_small), axis=0)
    local_large = jnp.cumsum(jax.nn.log_sigmoid(forget_large), axis=0)
    local = jnp.concatenate(
        [
            local_small.T.reshape(steps, per, rows),
            local_large.T.reshape(steps, 1, rows),
            jnp.zeros((steps, 7 - per, rows), jnp.float32),
        ],
        axis=1,
    ).reshape(steps * 8, rows)
    every, keys_s, values_s, keys_l, values_l, gate_full, up_full, down_blocks = gather_all(
        [local, k_small, v_small, k_large, v_large, w_gate, w_up, w_down],
        [False, True, True, True, False, False, False, False],
    )
    flat = lambda x: x.reshape(-1, x.shape[-1])
    gate_full, up_full = flat(gate_full), flat(up_full)
    totals = every[:, :, -1]
    before = jnp.cumsum(totals, axis=0) - totals
    cum = (every + before[:, :, None]).transpose(1, 0, 2).reshape(steps * 8, -1)
    normed_small, normed_large = attention(
        cum, steps, per, q_small, keys_s, values_s, q_large, keys_l, values_l
    )
    first_part = jnp.dot(normed_small, w_out_small, preferred_element_type=jnp.float32)
    projected = sum_over_tp(
        first_part + jnp.dot(normed_large, w_out_large, preferred_element_type=jnp.float32), 1
    )
    first = residual.astype(jnp.float32) + projected
    normal = (
        first * lax.rsqrt(jnp.mean(first * first, axis=-1, keepdims=True) + EPS) * norm_gain
    ).astype(jnp.bfloat16)
    piece = flat(exchange(normal, False, 2))
    gate_part = jnp.dot(piece, gate_full, preferred_element_type=jnp.float32).astype(jnp.bfloat16)
    up_part = jnp.dot(piece, up_full, preferred_element_type=jnp.float32).astype(jnp.bfloat16)
    both = jnp.concatenate([gate_part, up_part], axis=1)
    width = both.shape[0]
    rim = from_behind(both[width - 2 :], "sp", 1)
    extended = jnp.concatenate([rim, both], axis=0).astype(jnp.float32)
    taps = jnp.concatenate([conv_gate, conv_up], axis=1)
    conv = (
        taps[0] * extended[0:width]
        + taps[1] * extended[1 : width + 1]
        + taps[2] * extended[2 : width + 2]
    )
    half = gate_full.shape[1]
    hidden = (jax.nn.silu(conv[:, :half]) * conv[:, half:]).astype(jnp.bfloat16)
    mixed = first + sum_over_tp(down_product(hidden, down_blocks), 3)
    return mixed.astype(jnp.bfloat16)


def solution(mesh):
    placed = (
        P(("sp", "tp"), None),
        P("sp", "tp"),
        P("sp", "tp"),
        P("sp", "tp"),
        P("sp", "tp"),
        P("sp", "tp"),
        P("sp", "tp"),
        P("sp", "tp"),
        P("sp", "tp"),
        P("tp", None),
        P("tp", None),
        P(),
        P("sp", "tp"),
        P("sp", "tp"),
        P(None, "tp"),
        P(None, "tp"),
        P("tp", "sp"),
    )
    return jax.shard_map(
        body, mesh=mesh, in_specs=placed, out_specs=P(("sp", "tp"), None), check_vma=False
    )
```
